32 devices in a mesh: grp: 2 (over y), ep: 8 (over z, core), tp: 2 (over x).
Axes of the slice: x: 2, y: 2, z: 4, core: 2. Of those that a mesh axis runs over, the one named last changes fastest.
Arguments:
- tokens: bfloat16 [512, 2048], P(('grp', 'ep')), parts along dimension 0, may hold values from -12 to 12
- routes: int32 [512, 4], P(('grp', 'ep')), parts along dimension 0, may hold values from 0 to 7, all different within a row; in each aligned block of 32 rows (0 to 31, 32 to 63, ...) at most 32 rows name the same one
- gates: float32 [512, 4], P(('grp', 'ep')), parts along dimension 0, may hold values from 0.1 to 1
- norm_gain: bfloat16 [2048], replicated, may hold values from 0.099609375 to 1.8984375
- exp_gate: bfloat16 [8, 2048, 2048], P('ep', None, 'tp'), may hold values from -0.125 to 0.125
- exp_up: bfloat16 [8, 2048, 2048], P('ep', None, 'tp'), may hold values from -0.125 to 0.125
- exp_down: bfloat16 [8, 2048, 2048], P('ep', 'tp'), may hold values from -0.26516504 to 0.26516504
- sh_gate: bfloat16 [2048, 1024], P(None, 'tp'), may hold values from -0.125 to 0.125
- sh_up: bfloat16 [2048, 1024], P(None, 'tp'), may hold values from -0.125 to 0.125
- sh_down: bfloat16 [1024, 2048], P('tp'), may hold values from -0.375 to 0.375
- out_gain: bfloat16 [2048], P('tp'), may hold values from 0.099609375 to 1.8984375
Outputs:
- mixed: bfloat16 [512, 2048], P(('grp', 'ep'), 'tp'), parts along dimension 0
The draws below stay inside these ranges and needn't reach their ends.
There are 2 independent parts, one for each index of `grp`. The reference program is written for one: setup_inputs(seed, part) draws one part's arguments, and reference() takes and returns one part's arrays. A program takes and returns all parts, laid end to end along the dimension named above; an argument that names none is the same for every part. Nothing has to cross between parts.
Inputs may be any that keep to these rules, and one draw needn't show every extreme that they name: `routes`: each row names 4 different experts; within the rows of one device (aligned blocks of 32 rows) no expert is named by more than 32 rows, a bound that some block reaches.
All inputs are finite; a program needn't handle non-finite values.
Results may differ from the reference program's by a relative error of at most 0.015.
Values may be sent and summed in bfloat16 or wider, within the bound.
A program may use at most 64 MiB of HBM per device.

```python
import math
import jax
import jax.numpy as jnp
import numpy as np
from jax import lax

D = 2048
FF = 2048
SHARED_FF = 1024
TOP_K = 4
TOK_EP = 32
EXPERTS = 8
TOKENS = 256
CAP = 32
N_EP = 8
N_TP = 2


def rising_down(key, array_shape, fan_in):
    column = jnp.arange(D, dtype=jnp.float32) / (D - 1)
    base_draw = jnp.clip(jax.random.normal(key, array_shape, jnp.float32), -4.0, 4.0)
    profile = 5.0 ** (column - 0.5)
    return (base_draw * profile * fan_in ** (-0.5)).astype(jnp.bfloat16)


def draw_exp_down(key, part):
    return rising_down(jax.random.fold_in(key, 11), (EXPERTS, FF, D), FF)


def draw_sh_down(key, part):
    return rising_down(jax.random.fold_in(key, 23), (SHARED_FF, D), SHARED_FF)


def shard_levels(own_key, extent, cuts, least, top_value):
    def one(dim, blocks):
        heights = jax.random.uniform(jax.random.fold_in(jax.random.fold_in(own_key, 6), dim), (blocks,), jnp.float32, least / len(cuts), top_value / len(cuts))
        return jnp.repeat(jnp.exp(heights), extent[dim] // blocks).reshape((-1,) + (1,) * (len(extent) - dim - 1))

    factor_of = one(*cuts[0])
    for cut in cuts[1:]:
        factor_of = factor_of * one(*cut)
    return factor_of


def shared_out(rng, own, number, rows, amount, top, most, skew):
    ranking = jax.random.permutation(rng, amount)
    packed, usual = load_shares(amount, rows * top, most, skew, True), load_shares(amount, rows * top, most, skew, False)
    places = jnp.arange(amount)

    def named(sizes, rotation):
        used = int((sizes > 0).sum())
        fixed = max(1, used // 4)
        moved = fixed + (places - fixed + rotation * (used - fixed)) % max(1, amount - fixed)
        return jnp.zeros((amount,), jnp.int32).at[ranking[jnp.where(places < fixed, places, moved)]].set(jnp.asarray(sizes, jnp.int32))

    sizes = jnp.where(number % 4 == 0, named(packed, number // 4), named(usual, number - number // 4 - 1))
    mixed = jax.random.permutation(jax.random.fold_in(own, 3), amount)
    giver, receiver = mixed[0:amount // 2 * 2:2], mixed[1:amount // 2 * 2:2]
    margin = jnp.minimum(sizes[giver] - 1, most - sizes[receiver]) // 2
    margin = jnp.where((giver == ranking[0]) | (receiver == ranking[0]) | (sizes[receiver] == 0), 0, jnp.maximum(margin, 0))
    moved = jax.random.randint(jax.random.fold_in(own, 4), (amount // 2,), 0, 1 << 20) % (margin + 1)
    sizes = sizes.at[giver].add(-moved).at[receiver].add(moved)
    labels = jnp.searchsorted(jnp.cumsum(sizes), jnp.arange(rows * top), side="right").astype(jnp.int32)
    listing = labels.reshape(top, rows).T
    listing = listing[jax.random.permutation(jax.random.fold_in(own, 1), rows)]
    rotation = jax.random.randint(jax.random.fold_in(own, 2), (rows, 1), 0, top)
    return jnp.take_along_axis(listing, (jnp.arange(top)[None, :] + rotation) % top, axis=1)


def load_shares(count, total, reach, slope, full):
    portions = [(1 << 20) // math.isqrt(standing ** slope) + 1 for standing in range(1, count + 1)]
    largest = reach if full else min(reach, max(-(-total // count), total * portions[0] // sum(portions)))
    least = 1 if total - largest >= count - 1 else 0
    given, surplus = [largest] + [least] * (count - 1), total - largest - least * (count - 1)
    while surplus > 0:
        movable = [i for i in range(1, count) if given[i] < largest] or [i for i in range(1, count) if given[i] < reach]
        pool, budget = sum([portions[i] for i in movable]), surplus
        for i in movable:
            extra = min(reach - given[i], max(1, budget * portions[i] // pool), surplus)
            given[i] = given[i] + extra
            surplus = surplus - extra
    return np.array(given)


def normal_values(stream_key, dims, scale, reach, cuts=(), held_as=jnp.bfloat16):
    result = jax.random.normal(stream_key, dims, jnp.float32) * scale
    if len(cuts) > 0:
        result = shard_levels(stream_key, dims, cuts, -0.22, 0.18) * result
    return jnp.clip(result, min=-reach, max=reach).astype(held_as)


def setup_inputs(seed: int = 0, part: int = 0) -> dict:
    seeds = jax.random.split(jax.random.key(seed), 12)
    part_keys = jax.random.split(jax.random.fold_in(seeds[11], part), 12)
    tokens = normal_values(part_keys[0], (TOKENS, D), 2.0, 12.0, ((0, 8),))
    routes_keys = jax.random.split(jax.random.fold_in(part_keys[1], 1), TOKENS // TOK_EP)
    routes_turns = jax.random.permutation(jax.random.fold_in(part_keys[1], 3), TOKENS // TOK_EP)
    routes = jax.vmap(lambda own, number: shared_out(jax.random.fold_in(part_keys[1], 2), own, number, TOK_EP, EXPERTS, TOP_K, CAP, 2))(routes_keys, routes_turns).reshape((TOKENS, TOP_K))
    gates = jnp.clip(jnp.exp(math.log(1.0) - 2.3025851 * jax.random.uniform(part_keys[2], (TOKENS, TOP_K), jnp.float32) ** shard_levels(part_keys[2], (TOKENS, TOP_K), ((0, 8),), -0.2, 0.2)), 0.1, 1.0)
    norm_gain = jnp.clip(1.0 + 0.18 * jax.random.normal(seeds[3], (D,), jnp.float32), 0.099609375, 1.8984375).astype(jnp.bfloat16)
    exp_gate = normal_values(seeds[4], (EXPERTS, D, FF), D ** -0.5, 0.125, ((0, 8), (2, 2)))
    exp_up = normal_values(seeds[5], (EXPERTS, D, FF), D ** -0.5, 0.125, ((0, 8), (2, 2)))
    exp_down = draw_exp_down(jax.random.fold_in(seeds[11], 71), part)
    sh_gate = normal_values(seeds[7], (D, SHARED_FF), D ** -0.5, 0.125, ((1, 2),))
    sh_up = normal_values(seeds[8], (D, SHARED_FF), D ** -0.5, 0.125, ((1, 2),))
    sh_down = draw_sh_down(jax.random.fold_in(seeds[11], 71), part)
    out_gain = jnp.clip(1.0 + 0.18 * jax.random.normal(seeds[10], (D,), jnp.float32), 0.099609375, 1.8984375).astype(jnp.bfloat16)
    return {"tokens": tokens, "routes": routes, "gates": gates, "norm_gain": norm_gain, "exp_gate": exp_gate, "exp_up": exp_up, "exp_down": exp_down, "sh_gate": sh_gate, "sh_up": sh_up, "sh_down": sh_down, "out_gain": out_gain}


EPSILON = 1e-06

def slot_order(flat_routes, count):
    hits = (flat_routes[:, None] == jnp.arange(count, dtype=jnp.int32)[None, :]).astype(jnp.int32)
    before = jnp.cumsum(hits, axis=0) - hits
    return lax.optimization_barrier(jnp.sum(before * hits, axis=1)).astype(jnp.int32)

def swiglu_blocks(row_block, w_gate, w_up, w_down):
    gate_act = jnp.dot(row_block, w_gate, preferred_element_type=jnp.float32)
    up_act = jnp.dot(row_block, w_up, preferred_element_type=jnp.float32)
    hidden = (jax.nn.silu(gate_act) * up_act).astype(jnp.bfloat16)
    width = w_down.shape[0] // N_TP
    pieces = jnp.einsum('rnf,nfd->nrd', hidden.astype(jnp.float32).reshape(row_block.shape[0], N_TP, width), w_down.astype(jnp.float32).reshape(N_TP, width, w_down.shape[1]))
    rounded = lax.optimization_barrier(pieces.astype(jnp.bfloat16)).astype(jnp.float32)
    return lax.optimization_barrier(jnp.sum(rounded, axis=0)).astype(jnp.bfloat16)

def reference(tokens, routes, gates, norm_gain, exp_gate, exp_up, exp_down, sh_gate, sh_up, sh_down, out_gain):
    values = tokens.astype(jnp.float32)
    normed = (values * lax.rsqrt(lax.optimization_barrier(jnp.mean(values * values, axis=1, keepdims=True)) + EPSILON) * norm_gain.astype(jnp.float32)).astype(jnp.bfloat16)
    flat_expert = routes.reshape(-1).astype(jnp.int32)
    slot_index = jax.vmap(lambda block_routes: slot_order(block_routes, EXPERTS))(routes.reshape(N_EP, TOK_EP * TOP_K).astype(jnp.int32)).reshape(-1)
    flat_token = jnp.repeat(jnp.arange(TOKENS, dtype=jnp.int32), TOP_K)
    source = flat_token // TOK_EP
    position = flat_expert * (N_EP * CAP) + source * CAP + slot_index
    token_table = jnp.zeros((EXPERTS * N_EP * CAP,), jnp.int32).at[position].set(flat_token)
    weight_table = jnp.zeros((EXPERTS * N_EP * CAP,), jnp.float32).at[position].set(gates.reshape(-1))

    def one_expert(inputs):
        token_index, w_gate, w_up, w_down = inputs
        return swiglu_blocks(normed[token_index], w_gate, w_up, w_down)
    outputs = lax.map(one_expert, (token_table.reshape(EXPERTS, N_EP * CAP), exp_gate, exp_up, exp_down))
    routed = jnp.zeros((TOKENS, D), jnp.float32).at[token_table].add(weight_table[:, None] * outputs.reshape(-1, D).astype(jnp.float32))
    shared = swiglu_blocks(normed, sh_gate, sh_up, sh_down).astype(jnp.float32)
    total = routed + shared
    scale = lax.rsqrt(lax.optimization_barrier(jnp.mean(total * total, axis=1, keepdims=True)) + EPSILON)
    return (total * scale * out_gain.astype(jnp.float32)).astype(jnp.bfloat16)
```

```python
import functools

import jax
import jax.numpy as jnp
from jax import lax
from jax.experimental import pallas as pl
from jax.experimental.pallas import tpu as pltpu
from jax.sharding import PartitionSpec as P

EPSILON = 1e-06
MESH = pl.DeviceIdType.MESH
F32 = jnp.float32
BF16 = jnp.bfloat16


def silu(v):
    return v / (1.0 + jnp.exp(-v))


def kernel(
    n_ep, n_tp, experts,
    tok_ref, routes_ref, gates_ref, ngain_ref, wg_hbm, wu_hbm, wd_hbm, sg_hbm, su_hbm, sd_hbm, ogain_ref,
    out_ref,
    wg, wu, wd, sg, su, sd, xs, hid, shid, shp, d_out, d_in, x_out, x_in, acc, z_out, z_in, q_out, q_in,
    w_sem, disp_send, disp_recv, fwd_send, fwd_recv, d_send, d_recv, x_send, x_recv, z_send, z_recv, q_send, q_recv,
):
    nz = n_ep // 2
    me = lax.axis_index("ep")
    t = lax.axis_index("tp")
    z, c = me // 2, lax.rem(me, 2)
    other = 1 - c
    T, D = tok_ref.shape
    F = wg.shape[1]
    S = sg.shape[1]
    Dt = D // n_tp
    rows = 2 * T
    pad = xs.shape[3] - D

    loads = []
    for i, (src, dst) in enumerate(
        ((sg_hbm, sg), (su_hbm, su), (sd_hbm, sd), (wg_hbm.at[0], wg), (wu_hbm.at[0], wu), (wd_hbm.at[0], wd))
    ):
        copy = pltpu.make_async_copy(src, dst, w_sem.at[i])
        copy.start()
        loads.append(copy)

    def zpeer(dz):
        peer = z
        for bit in range(dz.bit_length()):
            if dz >> bit & 1:
                peer = peer + (1 << bit) * (1 - 2 * lax.rem(z // (1 << bit), 2))
        return peer

    def tpeer(j):
        return lax.rem(t + j, n_tp)

    partner = {"ep": z * 2 + other}
    barrier = pltpu.get_barrier_semaphore()
    peers = [{"ep": zpeer(dz) * 2 + c} for dz in range(1, nz)] + [partner]
    peers += [{"tp": tpeer(j)} for j in range(1, n_tp)]
    for peer in peers:
        pl.semaphore_signal(barrier, inc=1, device_id=peer, device_id_type=MESH)

    def remote(src, dst, ssem, rsem, device):
        return pltpu.make_async_remote_copy(
            src_ref=src, dst_ref=dst, send_sem=ssem, recv_sem=rsem, device_id=device, device_id_type=MESH
        )

    values = tok_ref[...].astype(F32)
    scale = lax.rsqrt(jnp.mean(values * values, axis=1, keepdims=True) + EPSILON)
    normed = (values * scale * ngain_ref[...].astype(F32).reshape(1, D)).astype(BF16)
    row = lax.broadcasted_iota(jnp.int32, (pad, T), 0)
    row_expert = lax.rem(row, experts)
    dense = jnp.zeros((pad, T), F32)
    for k in range(routes_ref.shape[0]):
        dense = dense + jnp.where(row_expert == routes_ref[k : k + 1, :], gates_ref[k : k + 1, :], 0.0)
    high = dense.astype(BF16).astype(F32)
    rest = dense - high
    mid = rest.astype(BF16).astype(F32)
    part = row // experts
    packed = jnp.where(part == 0, high, jnp.where(part == 1, mid, jnp.where(part == 2, rest - mid, 0.0)))
    packed = packed.T
    xs[z, c, :, :D] = normed
    xs[z, c, :, D:] = packed.astype(BF16)

    pl.semaphore_wait(barrier, len(peers))

    sent = []

    def send(src, dst, ssem, rsem, device):
        copy = remote(src, dst, ssem, rsem, device)
        copy.start()
        sent.append(copy)
        return copy

    order = list(range(nz - 1, 0, -1))
    js = list(range(1, n_tp)) + [0]
    own = xs.at[z, c]
    for dz in order:
        send(own, own, disp_send.at[dz], disp_recv.at[dz], {"ep": zpeer(dz) * 2 + c})
    send(own, own, fwd_send.at[0], fwd_recv.at[0], partner)

    dtile = min(512, Dt)

    def shared():
        loads[0].wait()
        loads[1].wait()
        tile = min(256, S)

        @pl.loop(0, S // tile)
        def _(i):
            cols = pl.ds(pl.multiple_of(i * tile, tile), tile)
            x = xs[z, c, :, :D]
            g = jnp.dot(x, sg[:, cols], preferred_element_type=F32)
            u = jnp.dot(x, su[:, cols], preferred_element_type=F32)
            shid[:, cols] = (silu(g) * u).astype(BF16)

        loads[2].wait()

        @pl.loop(0, D // dtile)
        def _(i):
            cols = pl.ds(pl.multiple_of(i * dtile, dtile), dtile)
            shp[:, cols] = jnp.dot(shid[...], sd[:, cols], preferred_element_type=F32)

    def arrive(dz):
        block = xs.at[zpeer(dz), c]
        remote(block, block, disp_send.at[dz], disp_recv.at[dz], partner).wait_recv()
        send(block, block, fwd_send.at[dz], fwd_recv.at[dz], partner)

    ftile = min(512, F)
    glane = lax.broadcasted_iota(jnp.int32, (rows, pad), 1)
    mine = (lax.rem(glane, experts) == me) & (glane < 3 * experts)

    def hidden(dz):
        src_z = zpeer(dz)
        block = xs.at[src_z, other]
        remote(block, block, fwd_send.at[dz], fwd_recv.at[dz], partner).wait_recv()
        packed_gates = xs[src_z, :, :, D:].reshape(rows, pad).astype(F32)
        weight = jnp.sum(jnp.where(mine, packed_gates, 0.0), axis=1, keepdims=True)

        @pl.loop(0, F // ftile)
        def _(i):
            cols = pl.ds(pl.multiple_of(i * ftile, ftile), ftile)
            x = xs[src_z, :, :, :D].reshape(rows, D)
            g = jnp.dot(x, wg[:, cols], preferred_element_type=F32)
            u = jnp.dot(x, wu[:, cols], preferred_element_type=F32)
            hid[:, :, cols] = (silu(g) * u * weight).astype(BF16).reshape(2, T, ftile)

    def down(dz):
        src_z = zpeer(dz)
        for j in js:
            @pl.loop(0, Dt // dtile)
            def _(i):
                src = pl.ds(pl.multiple_of(tpeer(j) * Dt + i * dtile, dtile), dtile)
                dst = pl.ds(pl.multiple_of(i * dtile, dtile), dtile)
                h = hid[...].reshape(rows, F)
                both = jnp.dot(h, wd[:, src], preferred_element_type=F32).reshape(2, T, dtile)
                mine_first = c == 0
                keep = jnp.where(mine_first, both[0], both[1])
                give = jnp.where(mine_first, both[1], both[0])
                d_out[j, src_z, :, dst] = give.astype(BF16)
                if dz == 0:
                    keep = keep + shp[:, src]
                acc[j, src_z, :, dst] = keep

            send(d_out.at[j, src_z], d_in.at[j, src_z], d_send.at[j, dz], d_recv.at[j, dz], partner)

    def pair(dz):
        src_z = zpeer(dz)
        for j in js:
            remote(d_out.at[j, src_z], d_in.at[j, src_z], d_send.at[j, dz], d_recv.at[j, dz], partner).wait_recv()
            total = acc[j, src_z] + d_in[j, src_z].astype(F32)
            if j == 0:
                acc[0, src_z] = total
            else:
                x_out[j, src_z] = total.astype(BF16)
                send(x_out.at[j, src_z], x_in.at[j, src_z], x_send.at[j, dz], x_recv.at[j, dz], {"tp": tpeer(j)})

    def finish(dz):
        src_z = zpeer(dz)
        total = acc[0, src_z]
        for j in range(1, n_tp):
            remote(
                x_out.at[j, src_z], x_in.at[j, src_z], x_send.at[j, dz], x_recv.at[j, dz], {"tp": tpeer(j)}
            ).wait_recv()
            total = total + x_in[j, src_z].astype(F32)
        if dz == 0:
            acc[0, src_z] = total
        else:
            z_out[dz] = total.astype(BF16)
            send(z_out.at[dz], z_in.at[dz], z_send.at[dz], z_recv.at[dz], {"ep": src_z * 2 + c})

    shared()
    for load in loads[3:]:
        load.wait()
    hidden(0)
    down(0)
    slots = [0] + order
    for i, dz in enumerate(order):
        arrive(dz)
        pair(slots[i])
        hidden(dz)
        down(dz)
        if i:
            finish(slots[i - 1])
    pair(slots[-1])
    for dz in slots[-2:]:
        finish(dz)

    total = acc[0, z]
    for dz in order:
        remote(z_out.at[dz], z_in.at[dz], z_send.at[dz], z_recv.at[dz], partner).wait_recv()
        total = total + z_in[dz].astype(F32)
    squares = jnp.sum(total * total, axis=1, keepdims=True)
    q_out[...] = jnp.broadcast_to(squares, q_out.shape)
    q_copies = []
    for j in range(1, n_tp):
        q_copies.append(send(q_out, q_in.at[j], q_send.at[j], q_recv.at[j], {"tp": tpeer(j)}))
    gained = total * ogain_ref[...].astype(F32).reshape(1, Dt)
    for j, copy in enumerate(q_copies):
        copy.wait_recv()
        squares = squares + q_in[j + 1, :, :1]
    out_ref[...] = (gained * lax.rsqrt(squares / D + EPSILON)).astype(BF16)

    for copy in sent:
        copy.wait_send()


def solution(mesh):
    n_ep, n_tp = mesh.shape["ep"], mesh.shape["tp"]
    nz = n_ep // 2

    def shards(tokens, routes, gates, norm_gain, exp_gate, exp_up, exp_down, sh_gate, sh_up, sh_down, out_gain):
        T, D = tokens.shape
        local, _, F = exp_gate.shape
        S = sh_gate.shape[1]
        assert local == 1
        experts = local * n_ep
        Dt = D // n_tp
        pad = 128 * ((3 * experts + 127) // 128)
        vmem = pl.BlockSpec(memory_space=pltpu.VMEM)
        hbm = pl.BlockSpec(memory_space=pl.ANY)
        dma = pltpu.SemaphoreType.DMA
        return pl.pallas_call(
            functools.partial(kernel, n_ep, n_tp, experts),
            out_shape=jax.ShapeDtypeStruct((T, Dt), BF16),
            in_specs=[vmem] * 4 + [hbm] * 6 + [vmem],
            out_specs=vmem,
            scratch_shapes=[
                pltpu.VMEM((D, F), BF16),
                pltpu.VMEM((D, F), BF16),
                pltpu.VMEM((F, D), BF16),
                pltpu.VMEM((D, S), BF16),
                pltpu.VMEM((D, S), BF16),
                pltpu.VMEM((S, D), BF16),
                pltpu.VMEM((nz, 2, T, D + pad), BF16),
                pltpu.VMEM((2, T, F), BF16),
                pltpu.VMEM((T, S), BF16),
                pltpu.VMEM((T, D), F32),
                pltpu.VMEM((n_tp, nz, T, Dt), BF16),
                pltpu.VMEM((n_tp, nz, T, Dt), BF16),
                pltpu.VMEM((n_tp, nz, T, Dt), BF16),
                pltpu.VMEM((n_tp, nz, T, Dt), BF16),
                pltpu.VMEM((n_tp, nz, T, Dt), F32),
                pltpu.VMEM((nz, T, Dt), BF16),
                pltpu.VMEM((nz, T, Dt), BF16),
                pltpu.VMEM((T, 128), F32),
                pltpu.VMEM((n_tp, T, 128), F32),
                dma((6,)),
                dma((nz,)), dma((nz,)), dma((nz,)), dma((nz,)),
                dma((n_tp, nz)), dma((n_tp, nz)),
                dma((n_tp, nz)), dma((n_tp, nz)),
                dma((nz,)), dma((nz,)),
                dma((n_tp,)), dma((n_tp,)),
            ],
            compiler_params=pltpu.CompilerParams(collective_id=0, has_side_effects=True),
        )(
            tokens, routes.T, gates.T, norm_gain, exp_gate, exp_up, exp_down,
            sh_gate, sh_up, sh_down, out_gain,
        )

    placed = (
        P(("grp", "ep"), None),
        P(("grp", "ep"), None),
        P(("grp", "ep"), None),
        P(),
        P("ep", None, "tp"),
        P("ep", None, "tp"),
        P("ep", "tp", None),
        P(None, "tp"),
        P(None, "tp"),
        P("tp", None),
        P("tp"),
    )
    return jax.shard_map(
        shards, mesh=mesh, in_specs=placed, out_specs=P(("grp", "ep"), "tp"), check_vma=False
    )
```

```python
import functools

import jax
import jax.numpy as jnp
from jax import lax
from jax.experimental import pallas as pl
from jax.experimental.pallas import tpu as pltpu
from jax.sharding import PartitionSpec as P

EPSILON = 1e-06
MESH = pl.DeviceIdType.MESH
F32 = jnp.float32
BF16 = jnp.bfloat16


def silu(v):
    return v / (1.0 + jnp.exp(-v))


def kernel(
    n_ep, n_tp, experts,
    tok_hbm, routes_hbm, gates_hbm, ngain_hbm, wg_hbm, wu_hbm, wd_hbm, sg_hbm, su_hbm, sd_hbm, ogain_hbm,
    out_ref,
    tok, routes, gates, ngain, ogain,
    wg, wu, wd, sg, su, sd, xs, hid, shid, shp, d_out, d_in, x_out, x_in, acc, z_out, z_in, q_out, q_in,
    i_sem, w_sem, disp_send, disp_recv, pad_send, pad_recv, part_send, part_recv, fwd_send, fwd_recv,
    d_send, d_recv, x_send, x_recv, z_send, z_recv, q_send, q_recv,
):
    nz = n_ep // 2
    me = lax.axis_index("ep")
    t = lax.axis_index("tp")
    z, c = me // 2, lax.rem(me, 2)
    other = 1 - c
    T, D = tok.shape
    F = wg.shape[1]
    S = sg.shape[1]
    Dt = D // n_tp
    rows = nz * T
    pad = xs.shape[3] - D
    partner = {"ep": z * 2 + other}
    ks = list(range(1, nz))
    js = list(range(1, n_tp)) + [0]

    def tpeer(j):
        return lax.rem(t + j, n_tp)

    paired = jnp.minimum(z, nz - 1 - z)

    def distance(k):
        return jnp.where(k <= 2 * paired, (k + 1) // 2, k - paired)

    def source(k):
        if k == 0:
            return z
        to_left = jnp.where(k <= 2 * paired, k % 2 == 1, z > paired)
        return jnp.where(to_left, z - distance(k), z + distance(k))

    def seen(k):
        d, there = distance(k), source(k)
        rim = jnp.minimum(there, nz - 1 - there)
        return jnp.where(d > rim, d + rim, jnp.where(there > z, 2 * d - 1, 2 * d))

    def split(k):
        return 2 * distance(k) > nz

    barrier = pltpu.get_barrier_semaphore()
    peers = [{"ep": source(k) * 2 + c} for k in ks] + [partner] + [{"tp": tpeer(j)} for j in range(1, n_tp)]
    for peer in peers:
        pl.semaphore_signal(barrier, inc=1, device_id=peer, device_id_type=MESH)

    def load(pairs, sems):
        copies = []
        for i, (a, b) in enumerate(pairs):
            copy = pltpu.make_async_copy(a, b, sems.at[i])
            copy.start()
            copies.append(copy)
        return copies

    inputs = load(
        ((tok_hbm, tok), (ngain_hbm, ngain), (routes_hbm, routes), (gates_hbm, gates), (ogain_hbm, ogain)), i_sem
    )
    for copy in inputs:
        copy.wait()
    loads = load(
        ((wg_hbm.at[0], wg), (wu_hbm.at[0], wu), (wd_hbm.at[0], wd), (sg_hbm, sg), (su_hbm, su), (sd_hbm, sd)), w_sem
    )

    def remote(a, b, ssem, rsem, device):
        return pltpu.make_async_remote_copy(
            src_ref=a, dst_ref=b, send_sem=ssem, recv_sem=rsem, device_id=device, device_id_type=MESH
        )

    sent = []

    def send(a, b, ssem, rsem, device):
        copy = remote(a, b, ssem, rsem, device)
        copy.start()
        sent.append(copy)

    values = tok[...].astype(F32)
    scale = lax.rsqrt(jnp.mean(values * values, axis=1, keepdims=True) + EPSILON)
    xs[c, 0, :, :D] = (values * scale * ngain[...].astype(F32).reshape(1, D)).astype(BF16)
    row = lax.broadcasted_iota(jnp.int32, (pad, T), 0)
    row_expert = lax.rem(row, experts)
    dense = jnp.zeros((pad, T), F32)
    for k in range(routes.shape[0]):
        dense = dense + jnp.where(row_expert == routes[k : k + 1, :], gates[k : k + 1, :], 0.0)
    high = dense.astype(BF16).astype(F32)
    rest = dense - high
    mid = rest.astype(BF16).astype(F32)
    part = row // experts
    packed = jnp.where(part == 0, high, jnp.where(part == 1, mid, jnp.where(part == 2, rest - mid, 0.0)))
    xs[c, 0, :, D:] = packed.T.astype(BF16)

    pl.semaphore_wait(barrier, len(peers))

    own = xs.at[c, 0]

    def pad_of(k):
        return xs.at[c, k, :, pl.ds(D, pad)]

    def part_of(k, owner):
        return xs.at[c, k, :, pl.ds(pl.multiple_of(owner * Dt, Dt), Dt)]

    def dispatch(k, wanted):
        device = {"ep": source(k) * 2 + c}
        slot = seen(k)

        @pl.when(wanted & split(k))
        def _():
            remote(part_of(0, t), part_of(slot, t), part_send.at[0, k], part_recv.at[0, slot], device).start()
            remote(pad_of(0), pad_of(slot), pad_send.at[k], pad_recv.at[slot], device).start()

        @pl.when(wanted & ~split(k))
        def _():
            remote(own, xs.at[c, slot], disp_send.at[k], disp_recv.at[slot], device).start()

    for k in ks[:2]:
        dispatch(k, distance(k) == 1)
    for k in ks[::-1]:
        dispatch(k, distance(k) > 1)
    send(own, own, fwd_send.at[0], fwd_recv.at[0], partner)

    dtile = min(512, Dt)

    def shared():
        loads[3].wait()
        loads[4].wait()
        tile = min(256, S)

        @pl.loop(0, S // tile)
        def _(i):
            cols = pl.ds(pl.multiple_of(i * tile, tile), tile)
            x = xs[c, 0, :, :D]
            g = jnp.dot(x, sg[:, cols], preferred_element_type=F32)
            u = jnp.dot(x, su[:, cols], preferred_element_type=F32)
            shid[:, cols] = (silu(g) * u).astype(BF16)

        loads[5].wait()

        @pl.loop(0, D // dtile)
        def _(i):
            cols = pl.ds(pl.multiple_of(i * dtile, dtile), dtile)
            shp[:, cols] = jnp.dot(shid[...], sd[:, cols], preferred_element_type=F32)

    def relay(k):
        @pl.when(split(k))
        def _():
            piece = part_of(k, t)
            remote(piece, piece, part_send.at[0, k], part_recv.at[0, k], partner).wait_recv()
            for j in range(1, n_tp):
                remote(piece, piece, part_send.at[j, k], part_recv.at[j, k], {"tp": tpeer(j)}).start()

    def forward(k):
        return remote(xs.at[c, k], xs.at[c, k], fwd_send.at[k], fwd_recv.at[k], partner)

    def arrive(k):
        @pl.when(split(k))
        def _():
            remote(pad_of(k), pad_of(k), pad_send.at[k], pad_recv.at[k], partner).wait_recv()
            for j in range(1, n_tp):
                piece = part_of(k, lax.rem(t - j + n_tp, n_tp))
                remote(piece, piece, part_send.at[j, k], part_recv.at[j, k], partner).wait_recv()

        @pl.when(~split(k))
        def _():
            block = xs.at[c, k]
            remote(block, block, disp_send.at[k], disp_recv.at[k], partner).wait_recv()

        forward(k).start()

    def swap(k):
        block = xs.at[other, k]
        remote(block, block, fwd_send.at[k], fwd_recv.at[k], partner).wait_recv()

    ftile = min(512, F)

    glane = lax.broadcasted_iota(jnp.int32, (rows, pad), 1)
    mine = (lax.rem(glane, experts) == me) & (glane < 3 * experts)

    def hidden(half):
        packed_gates = xs[half, :, :, D:].reshape(rows, pad).astype(F32)
        weight = jnp.sum(jnp.where(mine, packed_gates, 0.0), axis=1, keepdims=True)
        for i in range(F // ftile):
            cols = pl.ds(i * ftile, ftile)
            x = xs[half, :, :, :D].reshape(rows, D)
            g = jnp.dot(x, wg[:, cols], preferred_element_type=F32)
            u = jnp.dot(x, wu[:, cols], preferred_element_type=F32)
            hid[half, :, cols] = (silu(g) * u * weight).astype(BF16)

    tiles = list(range(Dt // dtile))

    def columns(j, i):
        return pl.ds(pl.multiple_of(tpeer(j) * Dt + i * dtile, dtile), dtile)

    def down(half, j, i):
        return jnp.dot(hid[half], wd[:, columns(j, i)], preferred_element_type=F32).reshape(nz, T, dtile)

    def pass_over(j, i, k):
        return remote(d_out.at[j, i, k], d_in.at[j, i, k], d_send.at[j, i, k], d_recv.at[j, i, k], partner)

    def give(j):
        for i in tiles:
            d_out[j, i] = down(other, j, i).astype(BF16)
            for k in range(nz):
                copy = pass_over(j, i, k)
                copy.start()
                sent.append(copy)

    def keep(j):
        for i in tiles:
            acc[j, i] = down(c, j, i)

    def cross(j, i, k):
        return remote(x_out.at[j, i, k], x_in.at[j, i, k], x_send.at[j, i, k], x_recv.at[j, i, k], {"tp": tpeer(j)})

    def pair(j, k):
        for i in tiles:
            pass_over(j, i, k).wait_recv()
            total = acc[j, i, k] + d_in[j, i, k].astype(F32)
            if k == 0:
                total = total + shp[:, columns(j, i)]
            if j == 0:
                acc[0, i, k] = total
            else:
                x_out[j, i, k] = total.astype(BF16)
                copy = cross(j, i, k)
                copy.start()
                sent.append(copy)

    def finish(k):
        for i in tiles:
            total = acc[0, i, k]
            for j in range(1, n_tp):
                cross(j, i, k).wait_recv()
                total = total + x_in[j, i, k].astype(F32)
            if k == 0:
                acc[0, i, k] = total
            else:
                z_out[k, :, i * dtile : (i + 1) * dtile] = total.astype(BF16)
        if k:
            slot = seen(k)
            send(z_out.at[k], z_in.at[slot], z_send.at[k], z_recv.at[slot], {"ep": source(k) * 2 + c})

    for k in ks[:1]:
        arrive(k)
    for k in ks:
        relay(k)
    for k in ks[1:]:
        arrive(k)
    for copy in loads[:2]:
        copy.wait()
    hidden(c)
    for k in [0] + ks:
        swap(k)
    hidden(other)
    loads[2].wait()
    far_first = ks[::-1]
    for n, j in enumerate(js):
        give(j)
        if n:
            for k in far_first:
                pair(js[n - 1], k)
        keep(j)
    for k in far_first:
        pair(js[-1], k)
    shared()
    for j in js:
        pair(j, 0)
    for k in far_first + [0]:
        finish(k)

    total = jnp.concatenate([acc[0, i, 0] for i in tiles], axis=1)
    for k in ks:
        remote(z_out.at[k], z_in.at[k], z_send.at[k], z_recv.at[k], partner).wait_recv()
        total = total + z_in[k].astype(F32)
    squares = jnp.sum(total * total, axis=1, keepdims=True)
    q_out[...] = jnp.broadcast_to(squares, q_out.shape)
    for j in range(1, n_tp):
        send(q_out, q_in.at[j], q_send.at[j], q_recv.at[j], {"tp": tpeer(j)})
    gained = total * ogain[...].astype(F32).reshape(1, Dt)
    for j in range(1, n_tp):
        remote(q_out, q_in.at[j], q_send.at[j], q_recv.at[j], partner).wait_recv()
        squares = squares + q_in[j, :, :1]
    out_ref[...] = (gained * lax.rsqrt(squares / D + EPSILON)).astype(BF16)

    for copy in sent:
        copy.wait_send()
    for k in ks:
        forward(k).wait_send()

        @pl.when(split(k))
        def _():
            remote(pad_of(0), pad_of(k), pad_send.at[k], pad_recv.at[k], partner).wait_send()
            for j in range(n_tp):
                remote(part_of(0, t), part_of(k, t), part_send.at[j, k], part_recv.at[j, k], partner).wait_send()

        @pl.when(~split(k))
        def _():
            remote(own, xs.at[c, k], disp_send.at[k], disp_recv.at[k], partner).wait_send()


def solution(mesh):
    n_ep, n_tp = mesh.shape["ep"], mesh.shape["tp"]
    nz = n_ep // 2

    def shards(tokens, routes, gates, norm_gain, exp_gate, exp_up, exp_down, sh_gate, sh_up, sh_down, out_gain):
        T, D = tokens.shape
        local, _, F = exp_gate.shape
        S = sh_gate.shape[1]
        assert local == 1
        experts = local * n_ep
        Dt = D // n_tp
        pad = 128 * ((3 * experts + 127) // 128)
        dtile = min(512, Dt)
        tiles = Dt // dtile
        vmem = pl.BlockSpec(memory_space=pltpu.VMEM)
        hbm = pl.BlockSpec(memory_space=pl.ANY)
        dma = pltpu.SemaphoreType.DMA
        return pl.pallas_call(
            functools.partial(kernel, n_ep, n_tp, experts),
            out_shape=jax.ShapeDtypeStruct((T, Dt), BF16),
            in_specs=[hbm] * 11,
            out_specs=vmem,
            scratch_shapes=[
                pltpu.VMEM(tokens.shape, BF16),
                pltpu.VMEM(routes.shape[::-1], jnp.int32),
                pltpu.VMEM(gates.shape[::-1], F32),
                pltpu.VMEM(norm_gain.shape, BF16),
                pltpu.VMEM(out_gain.shape, BF16),
                pltpu.VMEM((D, F), BF16),
                pltpu.VMEM((D, F), BF16),
                pltpu.VMEM((F, D), BF16),
                pltpu.VMEM((D, S), BF16),
                pltpu.VMEM((D, S), BF16),
                pltpu.VMEM((S, D), BF16),
                pltpu.VMEM((2, nz, T, D + pad), BF16),
                pltpu.VMEM((2, nz * T, F), BF16),
                pltpu.VMEM((T, S), BF16),
                pltpu.VMEM((T, D), F32),
                pltpu.VMEM((n_tp, tiles, nz, T, dtile), BF16),
                pltpu.VMEM((n_tp, tiles, nz, T, dtile), BF16),
                pltpu.VMEM((n_tp, tiles, nz, T, dtile), BF16),
                pltpu.VMEM((n_tp, tiles, nz, T, dtile), BF16),
                pltpu.VMEM((n_tp, tiles, nz, T, dtile), F32),
                pltpu.VMEM((nz, T, Dt), BF16),
                pltpu.VMEM((nz, T, Dt), BF16),
                pltpu.VMEM((T, 128), F32),
                pltpu.VMEM((n_tp, T, 128), F32),
                dma((5,)), dma((6,)),
                dma((nz,)), dma((nz,)), dma((nz,)), dma((nz,)),
                dma((n_tp, nz)), dma((n_tp, nz)),
                dma((nz,)), dma((nz,)),
                dma((n_tp, tiles, nz)), dma((n_tp, tiles, nz)),
                dma((n_tp, tiles, nz)), dma((n_tp, tiles, nz)),
                dma((nz,)), dma((nz,)),
                dma((n_tp,)), dma((n_tp,)),
            ],
            compiler_params=pltpu.CompilerParams(collective_id=0, has_side_effects=True),
        )(
            tokens, routes.T, gates.T, norm_gain, exp_gate, exp_up, exp_down,
            sh_gate, sh_up, sh_down, out_gain,
        )

    placed = (
        P(("grp", "ep"), None),
        P(("grp", "ep"), None),
        P(("grp", "ep"), None),
        P(),
        P("ep", None, "tp"),
        P("ep", None, "tp"),
        P("ep", "tp", None),
        P(None, "tp"),
        P(None, "tp"),
        P("tp", None),
        P("tp"),
    )
    return jax.shard_map(
        shards, mesh=mesh, in_specs=placed, out_specs=P(("grp", "ep"), "tp"), check_vma=False
    )
```

```python
import functools

import jax
import jax.numpy as jnp
from jax import lax
from jax.experimental import pallas as pl
from jax.experimental.pallas import tpu as pltpu
from jax.sharding import PartitionSpec as P

EPSILON = 1e-06
MESH = pl.DeviceIdType.MESH
F32 = jnp.float32
BF16 = jnp.bfloat16


def silu(v):
    return v / (1.0 + jnp.exp(-v))


def kernel(
    n_ep, n_tp, experts,
    tok_hbm, routes_hbm, gates_hbm, ngain_hbm, wg_hbm, wu_hbm, wd_hbm, sg_hbm, su_hbm, sd_hbm, ogain_hbm,
    out_ref,
    tok, routes, gates, ngain, ogain,
    wg, wu, wd, sg, su, sd, xs, hid, shid, shp, d_out, d_in, x_out, x_in, acc, z_out, z_in, q_out, q_in,
    i_sem, w_sem, disp_send, disp_recv, pad_send, pad_recv, part_send, part_recv, fwd_send, fwd_recv,
    d_send, d_recv, x_send, x_recv, z_send, z_recv, q_send, q_recv,
):
    nz = n_ep // 2
    me = lax.axis_index("ep")
    t = lax.axis_index("tp")
    z, c = me // 2, lax.rem(me, 2)
    other = 1 - c
    T, D = tok.shape
    F = wg.shape[1]
    S = sg.shape[1]
    Dt = D // n_tp
    rows = nz * T
    pad = xs.shape[3] - D
    partner = {"ep": z * 2 + other}
    ks = list(range(1, nz))
    js = list(range(1, n_tp)) + [0]

    def tpeer(j):
        return lax.rem(t + j, n_tp)

    paired = jnp.minimum(z, nz - 1 - z)

    def distance(k):
        return jnp.where(k <= 2 * paired, (k + 1) // 2, k - paired)

    def source(k):
        if k == 0:
            return z
        low = 2 * z < nz
        to_left = jnp.where(k <= 2 * paired, low if k % 2 else ~low, z > paired)
        return jnp.where(to_left, z - distance(k), z + distance(k))

    def seen(k):
        d, there = distance(k), source(k)
        rim = jnp.minimum(there, nz - 1 - there)
        outer = jnp.where(2 * there < nz, z < there, z > there)
        return jnp.where(d > rim, d + rim, jnp.where(outer, 2 * d - 1, 2 * d))

    def mirror(k):
        return source(k) + z == nz - 1

    def beyond(k):
        return ((2 * source(k) < nz) != (2 * z < nz)) & ~mirror(k)

    def near(k):
        return (2 * source(k) < nz) == (2 * z < nz)

    barrier = pltpu.get_barrier_semaphore()
    peers = [{"ep": source(k) * 2 + c} for k in ks] + [partner] + [{"tp": tpeer(j)} for j in range(1, n_tp)]
    for peer in peers:
        pl.semaphore_signal(barrier, inc=1, device_id=peer, device_id_type=MESH)

    def load(pairs, sems):
        copies = []
        for i, (a, b) in enumerate(pairs):
            copy = pltpu.make_async_copy(a, b, sems.at[i])
            copy.start()
            copies.append(copy)
        return copies

    inputs = load(
        ((tok_hbm, tok), (ngain_hbm, ngain), (routes_hbm, routes), (gates_hbm, gates), (ogain_hbm, ogain)), i_sem
    )
    for copy in inputs[:2]:
        copy.wait()
    loads = load(
        ((wg_hbm.at[0], wg), (wu_hbm.at[0], wu), (wd_hbm.at[0], wd), (sg_hbm, sg), (su_hbm, su), (sd_hbm, sd)), w_sem
    )

    def remote(a, b, ssem, rsem, device):
        return pltpu.make_async_remote_copy(
            src_ref=a, dst_ref=b, send_sem=ssem, recv_sem=rsem, device_id=device, device_id_type=MESH
        )

    sent = []

    def send(a, b, ssem, rsem, device):
        copy = remote(a, b, ssem, rsem, device)
        copy.start()
        sent.append(copy)

    values = tok[...].astype(F32)
    scale = lax.rsqrt(jnp.mean(values * values, axis=1, keepdims=True) + EPSILON)
    xs[c, 0, :, :D] = (values * scale * ngain[...].astype(F32).reshape(1, D)).astype(BF16)
    pl.semaphore_wait(barrier, len(peers))

    own = xs.at[c, 0]

    def pad_of(k):
        return xs.at[c, k, :, pl.ds(D, pad)]

    def part_of(k, owner):
        return xs.at[c, k, :, pl.ds(pl.multiple_of(owner * Dt, Dt), Dt)]

    def half_of(k, owner):
        return xs.at[c, k, :, pl.ds(pl.multiple_of(owner * (Dt // 2), Dt // 2), Dt // 2)]

    def rest_of(k):
        return xs.at[c, k, :, pl.ds(D // 2, D // 2 + pad)]

    def first_pieces(k):
        device, slot = {"ep": source(k) * 2 + c}, seen(k)

        @pl.when(mirror(k))
        def _():
            remote(part_of(0, t), part_of(slot, t), part_send.at[0, k], part_recv.at[0, slot], device).start()

        @pl.when(beyond(k))
        def _():
            remote(half_of(0, t), half_of(slot, t), part_send.at[0, k], part_recv.at[0, slot], device).start()

    def whole(k):
        device, slot = {"ep": source(k) * 2 + c}, seen(k)

        @pl.when(mirror(k))
        def _():
            remote(pad_of(0), pad_of(slot), pad_send.at[k], pad_recv.at[slot], device).start()

        @pl.when(near(k))
        def _():
            remote(own, xs.at[c, slot], disp_send.at[k], disp_recv.at[slot], device).start()

        @pl.when(beyond(k))
        def _():
            remote(rest_of(0), rest_of(slot), disp_send.at[k], disp_recv.at[slot], device).start()

    for k in ks:
        first_pieces(k)
    for copy in inputs[2:]:
        copy.wait()
    row = lax.broadcasted_iota(jnp.int32, (pad, T), 0)
    row_expert = lax.rem(row, experts)
    dense = jnp.zeros((pad, T), F32)
    for k in range(routes.shape[0]):
        dense = dense + jnp.where(row_expert == routes[k : k + 1, :], gates[k : k + 1, :], 0.0)
    high = dense.astype(BF16).astype(F32)
    rest = dense - high
    mid = rest.astype(BF16).astype(F32)
    part = row // experts
    packed = jnp.where(part == 0, high, jnp.where(part == 1, mid, jnp.where(part == 2, rest - mid, 0.0)))
    xs[c, 0, :, D:] = packed.T.astype(BF16)

    for k in ks:
        whole(k)
    send(own, own, fwd_send.at[0], fwd_recv.at[0], partner)

    dtile = min(512, Dt)

    def shared():
        loads[3].wait()
        loads[4].wait()
        tile = min(256, S)

        @pl.loop(0, S // tile)
        def _(i):
            cols = pl.ds(pl.multiple_of(i * tile, tile), tile)
            x = xs[c, 0, :, :D]
            g = jnp.dot(x, sg[:, cols], preferred_element_type=F32)
            u = jnp.dot(x, su[:, cols], preferred_element_type=F32)
            shid[:, cols] = (silu(g) * u).astype(BF16)

        loads[5].wait()

        @pl.loop(0, D // dtile)
        def _(i):
            cols = pl.ds(pl.multiple_of(i * dtile, dtile), dtile)
            shp[:, cols] = jnp.dot(shid[...], sd[:, cols], preferred_element_type=F32)

    def relay(k):
        def go(of):
            piece = of(k, t)
            remote(piece, piece, part_send.at[0, k], part_recv.at[0, k], partner).wait_recv()
            for j in range(1, n_tp):
                remote(piece, piece, part_send.at[j, k], part_recv.at[j, k], {"tp": tpeer(j)}).start()

        pl.when(mirror(k))(lambda: go(part_of))
        pl.when(beyond(k))(lambda: go(half_of))

    def forward(k):
        return remote(xs.at[c, k], xs.at[c, k], fwd_send.at[k], fwd_recv.at[k], partner)

    def arrive(k):
        def go(of):
            for j in range(1, n_tp):
                piece = of(k, lax.rem(t - j + n_tp, n_tp))
                remote(piece, piece, part_send.at[j, k], part_recv.at[j, k], partner).wait_recv()

        @pl.when(mirror(k))
        def _():
            remote(pad_of(k), pad_of(k), pad_send.at[k], pad_recv.at[k], partner).wait_recv()
            go(part_of)

        @pl.when(beyond(k))
        def _():
            go(half_of)
            remote(rest_of(k), rest_of(k), disp_send.at[k], disp_recv.at[k], partner).wait_recv()

        @pl.when(near(k))
        def _():
            block = xs.at[c, k]
            remote(block, block, disp_send.at[k], disp_recv.at[k], partner).wait_recv()

        forward(k).start()

    def swap(k):
        block = xs.at[other, k]
        remote(block, block, fwd_send.at[k], fwd_recv.at[k], partner).wait_recv()

    ftile = min(512, F)

    glane = lax.broadcasted_iota(jnp.int32, (rows, pad), 1)
    mine = (lax.rem(glane, experts) == me) & (glane < 3 * experts)

    def hidden(half):
        packed_gates = xs[half, :, :, D:].reshape(rows, pad).astype(F32)
        weight = jnp.sum(jnp.where(mine, packed_gates, 0.0), axis=1, keepdims=True)
        for i in range(F // ftile):
            cols = pl.ds(i * ftile, ftile)
            x = xs[half, :, :, :D].reshape(rows, D)
            g = jnp.dot(x, wg[:, cols], preferred_element_type=F32)
            u = jnp.dot(x, wu[:, cols], preferred_element_type=F32)
            hid[half, :, cols] = (silu(g) * u * weight).astype(BF16)

    tiles = list(range(Dt // dtile))

    def columns(j, i):
        return pl.ds(pl.multiple_of(tpeer(j) * Dt + i * dtile, dtile), dtile)

    def down(half, j, i):
        return jnp.dot(hid[half], wd[:, columns(j, i)], preferred_element_type=F32).reshape(nz, T, dtile)

    def pass_over(j, i, k):
        return remote(d_out.at[j, i, k], d_in.at[j, i, k], d_send.at[j, i, k], d_recv.at[j, i, k], partner)

    def give(j):
        for i in tiles:
            d_out[j, i] = down(other, j, i).astype(BF16)
            for k in range(nz):
                copy = pass_over(j, i, k)
                copy.start()
                sent.append(copy)

    def keep(j):
        for i in tiles:
            acc[j, i] = down(c, j, i)

    def cross(j, i, k):
        return remote(x_out.at[j, i, k], x_in.at[j, i, k], x_send.at[j, i, k], x_recv.at[j, i, k], {"tp": tpeer(j)})

    def pair(j, k):
        for i in tiles:
            pass_over(j, i, k).wait_recv()
            total = acc[j, i, k] + d_in[j, i, k].astype(F32)
            if k == 0:
                total = total + shp[:, columns(j, i)]
            if j == 0:
                acc[0, i, k] = total
            else:
                x_out[j, i, k] = total.astype(BF16)
                copy = cross(j, i, k)
                copy.start()
                sent.append(copy)

    def finish(k):
        for i in tiles:
            total = acc[0, i, k]
            for j in range(1, n_tp):
                cross(j, i, k).wait_recv()
                total = total + x_in[j, i, k].astype(F32)
            if k == 0:
                acc[0, i, k] = total
            else:
                z_out[i, k] = total.astype(BF16)
                slot = seen(k)
                send(
                    z_out.at[i, k], z_in.at[i, slot], z_send.at[i, k], z_recv.at[i, slot], {"ep": source(k) * 2 + c}
                )

    for k in ks:
        relay(k)
    for k in ks:
        arrive(k)
    for copy in loads[:2]:
        copy.wait()
    hidden(c)
    for k in [0] + ks:
        swap(k)
    hidden(other)
    loads[2].wait()
    far_first = ks[::-1]
    for n, j in enumerate(js):
        give(j)
        if n:
            for k in far_first:
                pair(js[n - 1], k)
        keep(j)
    for k in far_first:
        pair(js[-1], k)
    shared()
    for j in js:
        pair(j, 0)
    for k in far_first + [0]:
        finish(k)

    totals = [acc[0, i, 0] for i in tiles]
    for k in ks:
        for i in tiles:
            remote(z_out.at[i, k], z_in.at[i, k], z_send.at[i, k], z_recv.at[i, k], partner).wait_recv()
            totals[i] = totals[i] + z_in[i, k].astype(F32)
    total = jnp.concatenate(totals, axis=1)
    squares = jnp.sum(total * total, axis=1, keepdims=True)
    q_out[...] = jnp.broadcast_to(squares, q_out.shape)
    for j in range(1, n_tp):
        send(q_out, q_in.at[j], q_send.at[j], q_recv.at[j], {"tp": tpeer(j)})
    gained = total * ogain[...].astype(F32).reshape(1, Dt)
    for j in range(1, n_tp):
        remote(q_out, q_in.at[j], q_send.at[j], q_recv.at[j], partner).wait_recv()
        squares = squares + q_in[j, :, :1]
    out_ref[...] = (gained * lax.rsqrt(squares / D + EPSILON)).astype(BF16)

    for copy in sent:
        copy.wait_send()
    for k in ks:
        forward(k).wait_send()

        @pl.when(mirror(k))
        def _():
            remote(pad_of(0), pad_of(k), pad_send.at[k], pad_recv.at[k], partner).wait_send()
            for j in range(n_tp):
                remote(part_of(0, t), part_of(k, t), part_send.at[j, k], part_recv.at[j, k], partner).wait_send()

        @pl.when(beyond(k))
        def _():
            for j in range(n_tp):
                remote(half_of(0, t), half_of(k, t), part_send.at[j, k], part_recv.at[j, k], partner).wait_send()
            remote(rest_of(0), rest_of(k), disp_send.at[k], disp_recv.at[k], partner).wait_send()

        @pl.when(near(k))
        def _():
            remote(own, xs.at[c, k], disp_send.at[k], disp_recv.at[k], partner).wait_send()


def solution(mesh):
    n_ep, n_tp = mesh.shape["ep"], mesh.shape["tp"]
    nz = n_ep // 2

    def shards(tokens, routes, gates, norm_gain, exp_gate, exp_up, exp_down, sh_gate, sh_up, sh_down, out_gain):
        T, D = tokens.shape
        local, _, F = exp_gate.shape
        S = sh_gate.shape[1]
        assert local == 1
        experts = local * n_ep
        Dt = D // n_tp
        pad = 128 * ((3 * experts + 127) // 128)
        dtile = min(512, Dt)
        tiles = Dt // dtile
        vmem = pl.BlockSpec(memory_space=pltpu.VMEM)
        hbm = pl.BlockSpec(memory_space=pl.ANY)
        dma = pltpu.SemaphoreType.DMA
        return pl.pallas_call(
            functools.partial(kernel, n_ep, n_tp, experts),
            out_shape=jax.ShapeDtypeStruct((T, Dt), BF16),
            in_specs=[hbm] * 11,
            out_specs=vmem,
            scratch_shapes=[
                pltpu.VMEM(tokens.shape, BF16),
                pltpu.VMEM(routes.shape[::-1], jnp.int32),
                pltpu.VMEM(gates.shape[::-1], F32),
                pltpu.VMEM(norm_gain.shape, BF16),
                pltpu.VMEM(out_gain.shape, BF16),
                pltpu.VMEM((D, F), BF16),
                pltpu.VMEM((D, F), BF16),
                pltpu.VMEM((F, D), BF16),
                pltpu.VMEM((D, S), BF16),
                pltpu.VMEM((D, S), BF16),
                pltpu.VMEM((S, D), BF16),
                pltpu.VMEM((2, nz, T, D + pad), BF16),
                pltpu.VMEM((2, nz * T, F), BF16),
                pltpu.VMEM((T, S), BF16),
                pltpu.VMEM((T, D), F32),
                pltpu.VMEM((n_tp, tiles, nz, T, dtile), BF16),
                pltpu.VMEM((n_tp, tiles, nz, T, dtile), BF16),
                pltpu.VMEM((n_tp, tiles, nz, T, dtile), BF16),
                pltpu.VMEM((n_tp, tiles, nz, T, dtile), BF16),
                pltpu.VMEM((n_tp, tiles, nz, T, dtile), F32),
                pltpu.VMEM((tiles, nz, T, dtile), BF16),
                pltpu.VMEM((tiles, nz, T, dtile), BF16),
                pltpu.VMEM((T, 128), F32),
                pltpu.VMEM((n_tp, T, 128), F32),
                dma((5,)), dma((6,)),
                dma((nz,)), dma((nz,)), dma((nz,)), dma((nz,)),
                dma((n_tp, nz)), dma((n_tp, nz)),
                dma((nz,)), dma((nz,)),
                dma((n_tp, tiles, nz)), dma((n_tp, tiles, nz)),
                dma((n_tp, tiles, nz)), dma((n_tp, tiles, nz)),
                dma((tiles, nz)), dma((tiles, nz)),
                dma((n_tp,)), dma((n_tp,)),
            ],
            compiler_params=pltpu.CompilerParams(collective_id=0, has_side_effects=True),
        )(
            tokens, routes.T, gates.T, norm_gain, exp_gate, exp_up, exp_down,
            sh_gate, sh_up, sh_down, out_gain,
        )

    placed = (
        P(("grp", "ep"), None),
        P(("grp", "ep"), None),
        P(("grp", "ep"), None),
        P(),
        P("ep", None, "tp"),
        P("ep", None, "tp"),
        P("ep", "tp", None),
        P(None, "tp"),
        P(None, "tp"),
        P("tp", None),
        P("tp"),
    )
    return jax.shard_map(
        shards, mesh=mesh, in_specs=placed, out_specs=P(("grp", "ep"), "tp"), check_vma=False
    )
```

```python
import functools

import jax
import jax.numpy as jnp
from jax import lax
from jax.experimental import pallas as pl
from jax.experimental.pallas import tpu as pltpu
from jax.sharding import PartitionSpec as P

EPSILON = 1e-06
MESH = pl.DeviceIdType.MESH
F32 = jnp.float32
BF16 = jnp.bfloat16


def silu(v):
    return v / (1.0 + jnp.exp(-v))


def kernel(
    n_ep, n_tp, experts,
    tok_hbm, routes_hbm, gates_hbm, ngain_hbm, wg_hbm, wu_hbm, wd_hbm, sg_hbm, su_hbm, sd_hbm, ogain_hbm,
    out_ref,
    tok, routes, gates, ngain, ogain,
    wg, wu, wd, sg, su, sd, xs, hid, shid, shp, d_out, d_in, x_out, x_in, acc, z_out, z_in, q_out, q_in,
    i_sem, w_sem, disp_send, disp_recv, part_send, part_recv, fwd_send, fwd_recv,
    d_send, d_recv, x_send, x_recv, z_send, z_recv, q_send, q_recv,
):
    nz = n_ep // 2
    me = lax.axis_index("ep")
    t = lax.axis_index("tp")
    z, c = me // 2, lax.rem(me, 2)
    other = 1 - c
    T, D = tok.shape
    F = wg.shape[1]
    S = sg.shape[1]
    Dt = D // n_tp
    rows = nz * T
    pad = xs.shape[3] - D
    partner = {"ep": z * 2 + other}
    ks = list(range(1, nz))
    js = list(range(1, n_tp)) + [0]

    def tpeer(j):
        return lax.rem(t + j, n_tp)

    paired = jnp.minimum(z, nz - 1 - z)

    def distance(k):
        return jnp.where(k <= 2 * paired, (k + 1) // 2, k - paired)

    def source(k):
        if k == 0:
            return z
        low = 2 * z < nz
        to_left = jnp.where(k <= 2 * paired, low if k % 2 else ~low, z > paired)
        return jnp.where(to_left, z - distance(k), z + distance(k))

    def seen(k):
        d, there = distance(k), source(k)
        rim = jnp.minimum(there, nz - 1 - there)
        outer = jnp.where(2 * there < nz, z < there, z > there)
        return jnp.where(d > rim, d + rim, jnp.where(outer, 2 * d - 1, 2 * d))

    def beyond(k):
        return (2 * source(k) < nz) != (2 * z < nz)

    barrier = pltpu.get_barrier_semaphore()
    peers = [{"ep": source(k) * 2 + c} for k in ks] + [partner] + [{"tp": tpeer(j)} for j in range(1, n_tp)]
    for peer in peers:
        pl.semaphore_signal(barrier, inc=1, device_id=peer, device_id_type=MESH)

    def load(pairs, sems):
        copies = []
        for i, (a, b) in enumerate(pairs):
            copy = pltpu.make_async_copy(a, b, sems.at[i])
            copy.start()
            copies.append(copy)
        return copies

    inputs = load(
        ((tok_hbm, tok), (ngain_hbm, ngain), (routes_hbm, routes), (gates_hbm, gates), (ogain_hbm, ogain)), i_sem
    )
    for copy in inputs[:2]:
        copy.wait()
    loads = load(
        ((wg_hbm.at[0], wg), (wu_hbm.at[0], wu), (wd_hbm.at[0], wd), (sg_hbm, sg), (su_hbm, su), (sd_hbm, sd)), w_sem
    )

    def remote(a, b, ssem, rsem, device):
        return pltpu.make_async_remote_copy(
            src_ref=a, dst_ref=b, send_sem=ssem, recv_sem=rsem, device_id=device, device_id_type=MESH
        )

    sent = []

    def send(a, b, ssem, rsem, device):
        copy = remote(a, b, ssem, rsem, device)
        copy.start()
        sent.append(copy)

    values = tok[...].astype(F32)
    scale = lax.rsqrt(jnp.mean(values * values, axis=1, keepdims=True) + EPSILON)
    xs[c, 0, :, :D] = (values * scale * ngain[...].astype(F32).reshape(1, D)).astype(BF16)
    pl.semaphore_wait(barrier, len(peers))

    own = xs.at[c, 0]

    def half_of(k, owner):
        return xs.at[c, k, :, pl.ds(pl.multiple_of(owner * (Dt // 2), Dt // 2), Dt // 2)]

    def rest_of(k):
        return xs.at[c, k, :, pl.ds(D // 2, D // 2 + pad)]

    def first_pieces(k):
        device, slot = {"ep": source(k) * 2 + c}, seen(k)

        @pl.when(beyond(k))
        def _():
            remote(half_of(0, t), half_of(slot, t), part_send.at[0, k], part_recv.at[0, slot], device).start()

    def whole(k):
        device, slot = {"ep": source(k) * 2 + c}, seen(k)

        @pl.when(~beyond(k))
        def _():
            remote(own, xs.at[c, slot], disp_send.at[k], disp_recv.at[slot], device).start()

        @pl.when(beyond(k))
        def _():
            remote(rest_of(0), rest_of(slot), disp_send.at[k], disp_recv.at[slot], device).start()

    for k in ks:
        first_pieces(k)
    for copy in inputs[2:]:
        copy.wait()
    row = lax.broadcasted_iota(jnp.int32, (pad, T), 0)
    row_expert = lax.rem(row, experts)
    dense = jnp.zeros((pad, T), F32)
    for k in range(routes.shape[0]):
        dense = dense + jnp.where(row_expert == routes[k : k + 1, :], gates[k : k + 1, :], 0.0)
    high = dense.astype(BF16).astype(F32)
    rest = dense - high
    mid = rest.astype(BF16).astype(F32)
    part = row // experts
    packed = jnp.where(part == 0, high, jnp.where(part == 1, mid, jnp.where(part == 2, rest - mid, 0.0)))
    xs[c, 0, :, D:] = packed.T.astype(BF16)

    for k in ks:
        whole(k)
    send(own, own, fwd_send.at[0], fwd_recv.at[0], partner)

    dtile = min(512, Dt)

    def shared():
        loads[3].wait()
        loads[4].wait()
        tile = min(256, S)

        @pl.loop(0, S // tile)
        def _(i):
            cols = pl.ds(pl.multiple_of(i * tile, tile), tile)
            x = xs[c, 0, :, :D]
            g = jnp.dot(x, sg[:, cols], preferred_element_type=F32)
            u = jnp.dot(x, su[:, cols], preferred_element_type=F32)
            shid[:, cols] = (silu(g) * u).astype(BF16)

        loads[5].wait()

        @pl.loop(0, D // dtile)
        def _(i):
            cols = pl.ds(pl.multiple_of(i * dtile, dtile), dtile)
            shp[:, cols] = jnp.dot(shid[...], sd[:, cols], preferred_element_type=F32)

    def relay(k):
        @pl.when(beyond(k))
        def _():
            piece = half_of(k, t)
            remote(piece, piece, part_send.at[0, k], part_recv.at[0, k], partner).wait_recv()
            for j in range(1, n_tp):
                remote(piece, piece, part_send.at[j, k], part_recv.at[j, k], {"tp": tpeer(j)}).start()

    def forward(k):
        return remote(xs.at[c, k], xs.at[c, k], fwd_send.at[k], fwd_recv.at[k], partner)

    def arrive(k):
        @pl.when(beyond(k))
        def _():
            for j in range(1, n_tp):
                piece = half_of(k, lax.rem(t - j + n_tp, n_tp))
                remote(piece, piece, part_send.at[j, k], part_recv.at[j, k], partner).wait_recv()
            remote(rest_of(k), rest_of(k), disp_send.at[k], disp_recv.at[k], partner).wait_recv()

        @pl.when(~beyond(k))
        def _():
            block = xs.at[c, k]
            remote(block, block, disp_send.at[k], disp_recv.at[k], partner).wait_recv()

        forward(k).start()

    def swap(k):
        block = xs.at[other, k]
        remote(block, block, fwd_send.at[k], fwd_recv.at[k], partner).wait_recv()

    ftile = min(512, F)

    glane = lax.broadcasted_iota(jnp.int32, (rows, pad), 1)
    mine = (lax.rem(glane, experts) == me) & (glane < 3 * experts)

    def hidden(half):
        packed_gates = xs[half, :, :, D:].reshape(rows, pad).astype(F32)
        weight = jnp.sum(jnp.where(mine, packed_gates, 0.0), axis=1, keepdims=True)
        for i in range(F // ftile):
            cols = pl.ds(i * ftile, ftile)
            x = xs[half, :, :, :D].reshape(rows, D)
            g = jnp.dot(x, wg[:, cols], preferred_element_type=F32)
            u = jnp.dot(x, wu[:, cols], preferred_element_type=F32)
            hid[half, :, cols] = (silu(g) * u * weight).astype(BF16)

    tiles = list(range(Dt // dtile))

    def columns(j, i):
        return pl.ds(pl.multiple_of(tpeer(j) * Dt + i * dtile, dtile), dtile)

    def down(half, j, i):
        return jnp.dot(hid[half], wd[:, columns(j, i)], preferred_element_type=F32).reshape(nz, T, dtile)

    def pass_over(j, i, k):
        return remote(d_out.at[j, i, k], d_in.at[j, i, k], d_send.at[j, i, k], d_recv.at[j, i, k], partner)

    def give(j):
        for i in tiles:
            d_out[j, i] = down(other, j, i).astype(BF16)
            for k in ks[::-1] + [0]:
                copy = pass_over(j, i, k)
                copy.start()
                sent.append(copy)

    def keep(j):
        for i in tiles:
            acc[j, i] = down(c, j, i)

    def cross(j, i, k):
        return remote(x_out.at[j, i, k], x_in.at[j, i, k], x_send.at[j, i, k], x_recv.at[j, i, k], {"tp": tpeer(j)})

    def pair(j, k):
        for i in tiles:
            pass_over(j, i, k).wait_recv()
            total = acc[j, i, k] + d_in[j, i, k].astype(F32)
            if k == 0:
                total = total + shp[:, columns(j, i)]
            if j == 0:
                acc[0, i, k] = total
            else:
                x_out[j, i, k] = total.astype(BF16)
                copy = cross(j, i, k)
                copy.start()
                sent.append(copy)

    def finish(k):
        for i in tiles:
            total = acc[0, i, k]
            for j in range(1, n_tp):
                cross(j, i, k).wait_recv()
                total = total + x_in[j, i, k].astype(F32)
            if k == 0:
                acc[0, i, k] = total
            else:
                z_out[i, k] = total.astype(BF16)
                slot = seen(k)
                send(
                    z_out.at[i, k], z_in.at[i, slot], z_send.at[i, k], z_recv.at[i, slot], {"ep": source(k) * 2 + c}
                )

    for k in ks:
        relay(k)
    for k in ks:
        arrive(k)
    for copy in loads[:2]:
        copy.wait()
    hidden(c)
    for k in [0] + ks:
        swap(k)
    hidden(other)
    loads[2].wait()
    far_first = ks[::-1]
    for n, j in enumerate(js):
        give(j)
        if n:
            for k in far_first:
                pair(js[n - 1], k)
        keep(j)
    for k in far_first:
        pair(js[-1], k)
    shared()
    for j in js:
        pair(j, 0)
    for k in far_first + [0]:
        finish(k)

    totals = [acc[0, i, 0] for i in tiles]
    for k in ks:
        for i in tiles:
            remote(z_out.at[i, k], z_in.at[i, k], z_send.at[i, k], z_recv.at[i, k], partner).wait_recv()
            totals[i] = totals[i] + z_in[i, k].astype(F32)
    total = jnp.concatenate(totals, axis=1)
    squares = jnp.sum(total * total, axis=1, keepdims=True)
    q_out[...] = jnp.broadcast_to(squares, q_out.shape)
    for j in range(1, n_tp):
        send(q_out, q_in.at[j], q_send.at[j], q_recv.at[j], {"tp": tpeer(j)})
    gained = total * ogain[...].astype(F32).reshape(1, Dt)
    for j in range(1, n_tp):
        remote(q_out, q_in.at[j], q_send.at[j], q_recv.at[j], partner).wait_recv()
        squares = squares + q_in[j, :, :1]
    out_ref[...] = (gained * lax.rsqrt(squares / D + EPSILON)).astype(BF16)

    for copy in sent:
        copy.wait_send()
    for k in ks:
        forward(k).wait_send()

        @pl.when(beyond(k))
        def _():
            for j in range(n_tp):
                remote(half_of(0, t), half_of(k, t), part_send.at[j, k], part_recv.at[j, k], partner).wait_send()
            remote(rest_of(0), rest_of(k), disp_send.at[k], disp_recv.at[k], partner).wait_send()

        @pl.when(~beyond(k))
        def _():
            remote(own, xs.at[c, k], disp_send.at[k], disp_recv.at[k], partner).wait_send()


def solution(mesh):
    n_ep, n_tp = mesh.shape["ep"], mesh.shape["tp"]
    nz = n_ep // 2

    def shards(tokens, routes, gates, norm_gain, exp_gate, exp_up, exp_down, sh_gate, sh_up, sh_down, out_gain):
        T, D = tokens.shape
        local, _, F = exp_gate.shape
        S = sh_gate.shape[1]
        assert local == 1
        experts = local * n_ep
        Dt = D // n_tp
        pad = 128 * ((3 * experts + 127) // 128)
        dtile = min(512, Dt)
        tiles = Dt // dtile
        vmem = pl.BlockSpec(memory_space=pltpu.VMEM)
        hbm = pl.BlockSpec(memory_space=pl.ANY)
        dma = pltpu.SemaphoreType.DMA
        return pl.pallas_call(
            functools.partial(kernel, n_ep, n_tp, experts),
            out_shape=jax.ShapeDtypeStruct((T, Dt), BF16),
            in_specs=[hbm] * 11,
            out_specs=vmem,
            scratch_shapes=[
                pltpu.VMEM(tokens.shape, BF16),
                pltpu.VMEM(routes.shape[::-1], jnp.int32),
                pltpu.VMEM(gates.shape[::-1], F32),
                pltpu.VMEM(norm_gain.shape, BF16),
                pltpu.VMEM(out_gain.shape, BF16),
                pltpu.VMEM((D, F), BF16),
                pltpu.VMEM((D, F), BF16),
                pltpu.VMEM((F, D), BF16),
                pltpu.VMEM((D, S), BF16),
                pltpu.VMEM((D, S), BF16),
                pltpu.VMEM((S, D), BF16),
                pltpu.VMEM((2, nz, T, D + pad), BF16),
                pltpu.VMEM((2, nz * T, F), BF16),
                pltpu.VMEM((T, S), BF16),
                pltpu.VMEM((T, D), F32),
                pltpu.VMEM((n_tp, tiles, nz, T, dtile), BF16),
                pltpu.VMEM((n_tp, tiles, nz, T, dtile), BF16),
                pltpu.VMEM((n_tp, tiles, nz, T, dtile), BF16),
                pltpu.VMEM((n_tp, tiles, nz, T, dtile), BF16),
                pltpu.VMEM((n_tp, tiles, nz, T, dtile), F32),
                pltpu.VMEM((tiles, nz, T, dtile), BF16),
                pltpu.VMEM((tiles, nz, T, dtile), BF16),
                pltpu.VMEM((T, 128), F32),
                pltpu.VMEM((n_tp, T, 128), F32),
                dma((5,)), dma((6,)),
                dma((nz,)), dma((nz,)),
                dma((n_tp, nz)), dma((n_tp, nz)),
                dma((nz,)), dma((nz,)),
                dma((n_tp, tiles, nz)), dma((n_tp, tiles, nz)),
                dma((n_tp, tiles, nz)), dma((n_tp, tiles, nz)),
                dma((tiles, nz)), dma((tiles, nz)),
                dma((n_tp,)), dma((n_tp,)),
            ],
            compiler_params=pltpu.CompilerParams(collective_id=0, has_side_effects=True),
        )(
            tokens, routes.T, gates.T, norm_gain, exp_gate, exp_up, exp_down,
            sh_gate, sh_up, sh_down, out_gain,
        )

    placed = (
        P(("grp", "ep"), None),
        P(("grp", "ep"), None),
        P(("grp", "ep"), None),
        P(),
        P("ep", None, "tp"),
        P("ep", None, "tp"),
        P("ep", "tp", None),
        P(None, "tp"),
        P(None, "tp"),
        P("tp", None),
        P("tp"),
    )
    return jax.shard_map(
        shards, mesh=mesh, in_specs=placed, out_specs=P(("grp", "ep"), "tp"), check_vma=False
    )
```

```python
import functools

import jax
import jax.numpy as jnp
from jax import lax
from jax.experimental import pallas as pl
from jax.experimental.pallas import tpu as pltpu
from jax.sharding import PartitionSpec as P

EPSILON = 1e-06
MESH = pl.DeviceIdType.MESH
F32 = jnp.float32
BF16 = jnp.bfloat16


def silu(v):
    return v / (1.0 + jnp.exp(-v))


def kernel(
    n_ep, n_tp, experts,
    tok_hbm, routes_hbm, gates_hbm, ngain_hbm, wg_hbm, wu_hbm, wd_hbm, sg_hbm, su_hbm, sd_hbm, ogain_hbm,
    out_ref,
    tok, routes, gates, ngain, ogain,
    wg, wu, wd, sg, su, sd, xs, hid, shid, shp, d_out, d_in, x_out, x_in, acc, z_out, z_in, q_out, q_in,
    i_sem, w_sem, disp_send, disp_recv, part_send, part_recv, fwd_send, fwd_recv,
    d_send, d_recv, x_send, x_recv, z_send, z_recv, q_send, q_recv,
):
    nz = n_ep // 2
    me = lax.axis_index("ep")
    t = lax.axis_index("tp")
    z, c = me // 2, lax.rem(me, 2)
    other = 1 - c
    T, D = tok.shape
    F = wg.shape[1]
    S = sg.shape[1]
    Dt = D // n_tp
    rows = nz * T
    pad = xs.shape[3] - D
    partner = {"ep": z * 2 + other}
    ks = list(range(1, nz))
    js = list(range(1, n_tp)) + [0]

    def tpeer(j):
        return lax.rem(t + j, n_tp)

    paired = jnp.minimum(z, nz - 1 - z)

    def distance(k):
        return jnp.where(k <= 2 * paired, (k + 1) // 2, k - paired)

    def source(k):
        if k == 0:
            return z
        low = 2 * z < nz
        to_left = jnp.where(k <= 2 * paired, low if k % 2 else ~low, z > paired)
        return jnp.where(to_left, z - distance(k), z + distance(k))

    def seen(k):
        d, there = distance(k), source(k)
        rim = jnp.minimum(there, nz - 1 - there)
        outer = jnp.where(2 * there < nz, z < there, z > there)
        return jnp.where(d > rim, d + rim, jnp.where(outer, 2 * d - 1, 2 * d))

    def beyond(k):
        return (2 * source(k) < nz) != (2 * z < nz)

    barrier = pltpu.get_barrier_semaphore()
    peers = [{"ep": source(k) * 2 + c} for k in ks] + [partner] + [{"tp": tpeer(j)} for j in range(1, n_tp)]
    for peer in peers:
        pl.semaphore_signal(barrier, inc=1, device_id=peer, device_id_type=MESH)

    def load(pairs, sems):
        copies = []
        for i, (a, b) in enumerate(pairs):
            copy = pltpu.make_async_copy(a, b, sems.at[i])
            copy.start()
            copies.append(copy)
        return copies

    inputs = load(
        ((tok_hbm, tok), (ngain_hbm, ngain), (routes_hbm, routes), (gates_hbm, gates), (ogain_hbm, ogain)), i_sem
    )
    for copy in inputs[:2]:
        copy.wait()
    loads = load(
        ((wg_hbm.at[0], wg), (wu_hbm.at[0], wu), (wd_hbm.at[0], wd), (sg_hbm, sg), (su_hbm, su), (sd_hbm, sd)), w_sem
    )

    def remote(a, b, ssem, rsem, device):
        return pltpu.make_async_remote_copy(
            src_ref=a, dst_ref=b, send_sem=ssem, recv_sem=rsem, device_id=device, device_id_type=MESH
        )

    sent = []

    def send(a, b, ssem, rsem, device):
        copy = remote(a, b, ssem, rsem, device)
        copy.start()
        sent.append(copy)

    values = tok[...].astype(F32)
    scale = lax.rsqrt(jnp.mean(values * values, axis=1, keepdims=True) + EPSILON)
    xs[c, 0, :, :D] = (values * scale * ngain[...].astype(F32).reshape(1, D)).astype(BF16)
    for copy in inputs[2:]:
        copy.wait()
    row = lax.broadcasted_iota(jnp.int32, (pad, T), 0)
    row_expert = lax.rem(row, experts)
    dense = jnp.zeros((pad, T), F32)
    for k in range(routes.shape[0]):
        dense = dense + jnp.where(row_expert == routes[k : k + 1, :], gates[k : k + 1, :], 0.0)
    high = dense.astype(BF16).astype(F32)
    rest = dense - high
    mid = rest.astype(BF16).astype(F32)
    part = row // experts
    packed = jnp.where(part == 0, high, jnp.where(part == 1, mid, jnp.where(part == 2, rest - mid, 0.0)))
    xs[c, 0, :, D:] = packed.T.astype(BF16)

    pl.semaphore_wait(barrier, len(peers))

    own = xs.at[c, 0]

    def half_of(k, owner):
        return xs.at[c, k, :, pl.ds(pl.multiple_of(owner * (Dt // 2), Dt // 2), Dt // 2)]

    def rest_of(k):
        return xs.at[c, k, :, pl.ds(D // 2, D // 2 + pad)]

    def first_pieces(k):
        device, slot = {"ep": source(k) * 2 + c}, seen(k)

        @pl.when(beyond(k))
        def _():
            remote(half_of(0, t), half_of(slot, t), part_send.at[0, k], part_recv.at[0, slot], device).start()

    def whole(k):
        device, slot = {"ep": source(k) * 2 + c}, seen(k)

        @pl.when(~beyond(k))
        def _():
            remote(own, xs.at[c, slot], disp_send.at[k], disp_recv.at[slot], device).start()

        @pl.when(beyond(k))
        def _():
            remote(rest_of(0), rest_of(slot), disp_send.at[k], disp_recv.at[slot], device).start()

    for k in ks:
        first_pieces(k)
    for k in ks:
        whole(k)
    send(own, own, fwd_send.at[0], fwd_recv.at[0], partner)

    dtile = min(512, Dt)

    def shared():
        loads[3].wait()
        loads[4].wait()
        tile = min(256, S)

        @pl.loop(0, S // tile)
        def _(i):
            cols = pl.ds(pl.multiple_of(i * tile, tile), tile)
            x = xs[c, 0, :, :D]
            g = jnp.dot(x, sg[:, cols], preferred_element_type=F32)
            u = jnp.dot(x, su[:, cols], preferred_element_type=F32)
            shid[:, cols] = (silu(g) * u).astype(BF16)

        loads[5].wait()

        @pl.loop(0, D // dtile)
        def _(i):
            cols = pl.ds(pl.multiple_of(i * dtile, dtile), dtile)
            shp[:, cols] = jnp.dot(shid[...], sd[:, cols], preferred_element_type=F32)

    def relay(k):
        @pl.when(beyond(k))
        def _():
            piece = half_of(k, t)
            remote(piece, piece, part_send.at[0, k], part_recv.at[0, k], partner).wait_recv()
            for j in range(1, n_tp):
                remote(piece, piece, part_send.at[j, k], part_recv.at[j, k], {"tp": tpeer(j)}).start()

    def forward(k):
        return remote(xs.at[c, k], xs.at[c, k], fwd_send.at[k], fwd_recv.at[k], partner)

    def arrive(k):
        @pl.when(beyond(k))
        def _():
            for j in range(1, n_tp):
                piece = half_of(k, lax.rem(t - j + n_tp, n_tp))
                remote(piece, piece, part_send.at[j, k], part_recv.at[j, k], partner).wait_recv()
            remote(rest_of(k), rest_of(k), disp_send.at[k], disp_recv.at[k], partner).wait_recv()

        @pl.when(~beyond(k))
        def _():
            block = xs.at[c, k]
            remote(block, block, disp_send.at[k], disp_recv.at[k], partner).wait_recv()

        forward(k).start()

    def swap(k):
        block = xs.at[other, k]
        remote(block, block, fwd_send.at[k], fwd_recv.at[k], partner).wait_recv()

    ftile = min(512, F)

    glane = lax.broadcasted_iota(jnp.int32, (rows, pad), 1)
    mine = (lax.rem(glane, experts) == me) & (glane < 3 * experts)

    def hidden(half):
        packed_gates = xs[half, :, :, D:].reshape(rows, pad).astype(F32)
        weight = jnp.sum(jnp.where(mine, packed_gates, 0.0), axis=1, keepdims=True)
        for i in range(F // ftile):
            cols = pl.ds(i * ftile, ftile)
            x = xs[half, :, :, :D].reshape(rows, D)
            g = jnp.dot(x, wg[:, cols], preferred_element_type=F32)
            u = jnp.dot(x, wu[:, cols], preferred_element_type=F32)
            hid[half, :, cols] = (silu(g) * u * weight).astype(BF16)

    tiles = list(range(Dt // dtile))

    def columns(j, i):
        return pl.ds(pl.multiple_of(tpeer(j) * Dt + i * dtile, dtile), dtile)

    def down(half, j, i):
        return jnp.dot(hid[half], wd[:, columns(j, i)], preferred_element_type=F32).reshape(nz, T, dtile)

    def pass_over(j, i, k):
        return remote(d_out.at[j, i, k], d_in.at[j, i, k], d_send.at[j, i, k], d_recv.at[j, i, k], partner)

    def give(j):
        for i in tiles:
            d_out[j, i] = down(other, j, i).astype(BF16)
            for k in ks[::-1] + [0]:
                copy = pass_over(j, i, k)
                copy.start()
                sent.append(copy)

    def keep(j):
        for i in tiles:
            acc[j, i] = down(c, j, i)

    def cross(j, i, k):
        return remote(x_out.at[j, i, k], x_in.at[j, i, k], x_send.at[j, i, k], x_recv.at[j, i, k], {"tp": tpeer(j)})

    def pair(j, k):
        for i in tiles:
            pass_over(j, i, k).wait_recv()
            total = acc[j, i, k] + d_in[j, i, k].astype(F32)
            if k == 0:
                total = total + shp[:, columns(j, i)]
            if j == 0:
                acc[0, i, k] = total
            else:
                x_out[j, i, k] = total.astype(BF16)
                copy = cross(j, i, k)
                copy.start()
                sent.append(copy)

    def finish(k):
        for i in tiles:
            total = acc[0, i, k]
            for j in range(1, n_tp):
                cross(j, i, k).wait_recv()
                total = total + x_in[j, i, k].astype(F32)
            if k == 0:
                acc[0, i, k] = total
            else:
                z_out[i, k] = total.astype(BF16)
                slot = seen(k)
                send(
                    z_out.at[i, k], z_in.at[i, slot], z_send.at[i, k], z_recv.at[i, slot], {"ep": source(k) * 2 + c}
                )

    for k in ks:
        relay(k)
    for k in ks:
        arrive(k)
    for copy in loads[:2]:
        copy.wait()
    hidden(c)
    for k in [0] + ks:
        swap(k)
    hidden(other)
    loads[2].wait()
    far_first = ks[::-1]
    for n, j in enumerate(js):
        give(j)
        if n:
            for k in far_first:
                pair(js[n - 1], k)
        keep(j)
    for k in far_first:
        pair(js[-1], k)
    shared()
    for j in js:
        pair(j, 0)
    for k in far_first + [0]:
        finish(k)

    totals = [acc[0, i, 0] for i in tiles]
    for k in ks:
        for i in tiles:
            remote(z_out.at[i, k], z_in.at[i, k], z_send.at[i, k], z_recv.at[i, k], partner).wait_recv()
            totals[i] = totals[i] + z_in[i, k].astype(F32)
    total = jnp.concatenate(totals, axis=1)
    squares = jnp.sum(total * total, axis=1, keepdims=True)
    q_out[...] = jnp.broadcast_to(squares, q_out.shape)
    for j in range(1, n_tp):
        send(q_out, q_in.at[j], q_send.at[j], q_recv.at[j], {"tp": tpeer(j)})
    gained = total * ogain[...].astype(F32).reshape(1, Dt)
    for j in range(1, n_tp):
        remote(q_out, q_in.at[j], q_send.at[j], q_recv.at[j], partner).wait_recv()
        squares = squares + q_in[j, :, :1]
    out_ref[...] = (gained * lax.rsqrt(squares / D + EPSILON)).astype(BF16)

    for copy in sent:
        copy.wait_send()
    for k in ks:
        forward(k).wait_send()

        @pl.when(beyond(k))
        def _():
            for j in range(n_tp):
                remote(half_of(0, t), half_of(k, t), part_send.at[j, k], part_recv.at[j, k], partner).wait_send()
            remote(rest_of(0), rest_of(k), disp_send.at[k], disp_recv.at[k], partner).wait_send()

        @pl.when(~beyond(k))
        def _():
            remote(own, xs.at[c, k], disp_send.at[k], disp_recv.at[k], partner).wait_send()


def solution(mesh):
    n_ep, n_tp = mesh.shape["ep"], mesh.shape["tp"]
    nz = n_ep // 2

    def shards(tokens, routes, gates, norm_gain, exp_gate, exp_up, exp_down, sh_gate, sh_up, sh_down, out_gain):
        T, D = tokens.shape
        local, _, F = exp_gate.shape
        S = sh_gate.shape[1]
        assert local == 1
        experts = local * n_ep
        Dt = D // n_tp
        pad = 128 * ((3 * experts + 127) // 128)
        dtile = min(512, Dt)
        tiles = Dt // dtile
        vmem = pl.BlockSpec(memory_space=pltpu.VMEM)
        hbm = pl.BlockSpec(memory_space=pl.ANY)
        dma = pltpu.SemaphoreType.DMA
        return pl.pallas_call(
            functools.partial(kernel, n_ep, n_tp, experts),
            out_shape=jax.ShapeDtypeStruct((T, Dt), BF16),
            in_specs=[hbm] * 11,
            out_specs=vmem,
            scratch_shapes=[
                pltpu.VMEM(tokens.shape, BF16),
                pltpu.VMEM(routes.shape[::-1], jnp.int32),
                pltpu.VMEM(gates.shape[::-1], F32),
                pltpu.VMEM(norm_gain.shape, BF16),
                pltpu.VMEM(out_gain.shape, BF16),
                pltpu.VMEM((D, F), BF16),
                pltpu.VMEM((D, F), BF16),
                pltpu.VMEM((F, D), BF16),
                pltpu.VMEM((D, S), BF16),
                pltpu.VMEM((D, S), BF16),
                pltpu.VMEM((S, D), BF16),
                pltpu.VMEM((2, nz, T, D + pad), BF16),
                pltpu.VMEM((2, nz * T, F), BF16),
                pltpu.VMEM((T, S), BF16),
                pltpu.VMEM((T, D), F32),
                pltpu.VMEM((n_tp, tiles, nz, T, dtile), BF16),
                pltpu.VMEM((n_tp, tiles, nz, T, dtile), BF16),
                pltpu.VMEM((n_tp, tiles, nz, T, dtile), BF16),
                pltpu.VMEM((n_tp, tiles, nz, T, dtile), BF16),
                pltpu.VMEM((n_tp, tiles, nz, T, dtile), F32),
                pltpu.VMEM((tiles, nz, T, dtile), BF16),
                pltpu.VMEM((tiles, nz, T, dtile), BF16),
                pltpu.VMEM((T, 128), F32),
                pltpu.VMEM((n_tp, T, 128), F32),
                dma((5,)), dma((6,)),
                dma((nz,)), dma((nz,)),
                dma((n_tp, nz)), dma((n_tp, nz)),
                dma((nz,)), dma((nz,)),
                dma((n_tp, tiles, nz)), dma((n_tp, tiles, nz)),
                dma((n_tp, tiles, nz)), dma((n_tp, tiles, nz)),
                dma((tiles, nz)), dma((tiles, nz)),
                dma((n_tp,)), dma((n_tp,)),
            ],
            compiler_params=pltpu.CompilerParams(collective_id=0, has_side_effects=True),
        )(
            tokens, routes.T, gates.T, norm_gain, exp_gate, exp_up, exp_down,
            sh_gate, sh_up, sh_down, out_gain,
        )

    placed = (
        P(("grp", "ep"), None),
        P(("grp", "ep"), None),
        P(("grp", "ep"), None),
        P(),
        P("ep", None, "tp"),
        P("ep", None, "tp"),
        P("ep", "tp", None),
        P(None, "tp"),
        P(None, "tp"),
        P("tp", None),
        P("tp"),
    )
    return jax.shard_map(
        shards, mesh=mesh, in_specs=placed, out_specs=P(("grp", "ep"), "tp"), check_vma=False
    )
```
